32 devices in a mesh: fs: 4 (over z), rep: 2 (over y), tp: 4 (over x, core).
Axes of the slice: x: 2, y: 2, z: 4, core: 2. Of those that a mesh axis runs over, the one named last changes fastest.
Arguments:
- saved_hidden: bfloat16 [7168, 2048], P(('fs', 'rep')), may hold values from -12 to 12
- grad_value: bfloat16 [7168, 1024], P(('fs', 'rep'), 'tp'), may hold values from -12 to 12
- saved_mixed: bfloat16 [7168, 1024], P(('fs', 'rep'), 'tp'), may hold values from -12 to 12
- grad_output: bfloat16 [7168, 2048], P(('fs', 'rep')), may hold values from -12 to 12
- basis_value: bfloat16 [2048, 128], replicated, may hold values from -0.5 to 0.5
- basis_output: bfloat16 [2048, 128], replicated, may hold values from -0.5 to 0.5
- weight_value: float32 [2048, 1024], P('fs', 'tp'), may hold values from -0.125 to 0.125
- weight_output: float32 [1024, 2048], P('tp', 'fs'), may hold values from -0.1875 to 0.1875
- first_value: float32 [128, 1024], P('fs', 'tp'), may hold values from -4 to 4
- second_value: float32 [128, 1024], P('fs', 'tp'), may hold values from 0.05 to 0.5
- first_output: float32 [128, 1024], P('fs', 'tp'), may hold values from -4 to 4
- second_output: float32 [128, 1024], P('fs', 'tp'), may hold values from 0.05 to 0.5
Outputs:
- step_value: float32 [2048, 1024], P('fs', 'tp')
- step_output: float32 [1024, 2048], P('tp', 'fs')
- new_weight_value: float32 [2048, 1024], P('fs', 'tp')
- new_weight_output: float32 [1024, 2048], P('tp', 'fs')
- copy_value: bfloat16 [2048, 1024], P(None, 'tp')
- copy_output: bfloat16 [1024, 2048], P('tp')
- new_first_value: float32 [128, 1024], P('fs', 'tp')
- new_second_value: float32 [128, 1024], P('fs', 'tp')
- new_first_output: float32 [128, 1024], P('fs', 'tp')
- new_second_output: float32 [128, 1024], P('fs', 'tp')
The draws below stay inside these ranges and needn't reach their ends.
All inputs are finite; a program needn't handle non-finite values.
Results may differ from the reference program's by a relative error of at most 0.0045.
Values may be sent and summed in bfloat16 or wider, within the bound.
A program may use at most 64 MiB of HBM per device.

```python
import math
import jax
import jax.numpy as jnp
from jax import lax

D = 2048
AW = 1024
RANK = 128
TOKENS = 7168


def field_values(key, row_total, col_total, rising_columns):
    key_noise = jax.random.fold_in(key, 0)
    length = col_total if rising_columns else row_total
    position = jnp.arange(length, dtype=jnp.float32) / max(length - 1, 1)
    noise_field = jnp.clip(jax.random.normal(key_noise, (row_total, col_total), jnp.float32), -4.0, 4.0)
    scales = jnp.exp(math.log(3.0) * position)
    if rising_columns:
        return noise_field * scales[None, :]
    return noise_field * scales[:, None]


def draw_saved_hidden(key, part):
    return field_values(jax.random.fold_in(key, 11), TOKENS, D, False).astype(jnp.bfloat16)


def draw_grad_value(key, part):
    return field_values(jax.random.fold_in(key, 23), TOKENS, AW, True).astype(jnp.bfloat16)


def draw_saved_mixed(key, part):
    return field_values(jax.random.fold_in(key, 37), TOKENS, AW, True).astype(jnp.bfloat16)


def draw_grad_output(key, part):
    return field_values(jax.random.fold_in(key, 41), TOKENS, D, False).astype(jnp.bfloat16)


def steps_of(own_key, extent, cuts, smallest, top_value):
    loudness = 1.0
    for axis_at, shards_of in cuts:
        heights = jax.random.uniform(jax.random.fold_in(jax.random.fold_in(own_key, 6), axis_at), (shards_of,), jnp.float32, smallest / len(cuts), top_value / len(cuts))
        loudness = loudness * jnp.repeat(jnp.exp(heights), extent[axis_at] // shards_of).reshape((-1,) + (1,) * (len(extent) - 1 - axis_at))
    return loudness


def centred(rng, dims, scale, most, cuts=(), held_as=jnp.bfloat16):
    result = scale * jax.random.normal(rng, dims, jnp.float32)
    if cuts:
        result = result * steps_of(rng, dims, cuts, -0.22, 0.18)
    return jnp.clip(result, -most, most).astype(held_as)


def setup_inputs(seed: int = 0) -> dict:
    streams_of = jax.random.split(jax.random.key(seed), 13)
    return {
        "saved_hidden": draw_saved_hidden(jax.random.fold_in(streams_of[12], 71), 0),
        "grad_value": draw_grad_value(jax.random.fold_in(streams_of[12], 71), 0),
        "saved_mixed": draw_saved_mixed(jax.random.fold_in(streams_of[12], 71), 0),
        "grad_output": draw_grad_output(jax.random.fold_in(streams_of[12], 71), 0),
        "basis_value": centred(streams_of[4], (D, RANK), RANK ** -0.5, 0.5),
        "basis_output": centred(streams_of[5], (D, RANK), RANK ** -0.5, 0.5),
        "weight_value": centred(streams_of[6], (D, AW), D ** -0.5, 0.125, ((0, 4), (1, 4)), jnp.float32),
        "weight_output": centred(streams_of[7], (AW, D), AW ** -0.5, 0.1875, ((0, 4), (1, 4)), jnp.float32),
        "first_value": centred(streams_of[8], (RANK, AW), 1.0, 4.0, ((0, 4), (1, 4)), jnp.float32),
        "second_value": jnp.clip(jnp.exp(math.log(0.5) - 2.3025851 * jax.random.uniform(streams_of[9], (RANK, AW), jnp.float32) ** steps_of(streams_of[9], (RANK, AW), ((0, 4), (1, 4)), -0.2, 0.2)), 0.05, 0.5),
        "first_output": centred(streams_of[10], (RANK, AW), 1.0, 4.0, ((0, 4), (1, 4)), jnp.float32),
        "second_output": jnp.clip(jnp.exp(math.log(0.5) - 2.3025851 * jax.random.uniform(streams_of[11], (RANK, AW), jnp.float32) ** steps_of(streams_of[11], (RANK, AW), ((0, 4), (1, 4)), -0.2, 0.2)), 0.05, 0.5),
    }


first_decay = 0.8
second_decay = 0.9
learning_rate = 0.02
norm_epsilon = 1e-06

def project(basis, gradient):
    return jnp.dot(basis.astype(jnp.float32).T, gradient, precision=lax.Precision.HIGHEST)

def moments(projected, first_old, second_old, clip_factor):
    scaled = clip_factor * projected
    first_new = first_decay * first_old + (1.0 - first_decay) * scaled
    second_new = second_decay * second_old + (1.0 - second_decay) * scaled * scaled
    return (first_new, second_new, first_new / jnp.sqrt(second_new))

def reference(saved_hidden, grad_value, saved_mixed, grad_output, basis_value, basis_output, weight_value, weight_output, first_value, second_value, first_output, second_output):
    gradient_value = jnp.dot(saved_hidden.T, grad_value, preferred_element_type=jnp.float32)
    gradient_output = jnp.dot(grad_output.T, saved_mixed, preferred_element_type=jnp.float32)
    projected_value = project(basis_value, gradient_value)
    projected_output = project(basis_output, gradient_output)
    squares = jnp.sum(projected_value * projected_value) + jnp.sum(projected_output * projected_output)
    mean_square = squares / (2 * RANK * AW)
    clip_factor = jnp.minimum(1.0, 1.0 / jnp.sqrt(mean_square + norm_epsilon))
    first_new_value, second_new_value, direction_value = moments(projected_value, first_value, second_value, clip_factor)
    first_new_output, second_new_output, direction_output = moments(projected_output, first_output, second_output, clip_factor)
    step_value = jnp.dot(basis_value.astype(jnp.float32), direction_value, precision=lax.Precision.HIGHEST)
    step_output = jnp.dot(basis_output.astype(jnp.float32), direction_output, precision=lax.Precision.HIGHEST).T
    new_weight_value = weight_value - learning_rate * step_value
    new_weight_output = weight_output - learning_rate * step_output
    return (step_value, step_output, new_weight_value, new_weight_output, new_weight_value.astype(jnp.bfloat16), new_weight_output.astype(jnp.bfloat16), first_new_value, second_new_value, first_new_output, second_new_output)
```

```python
import functools
import jax
import jax.numpy as jnp
from jax import lax
from jax.experimental import pallas as pl
from jax.experimental.pallas import tpu as pltpu
from jax.sharding import PartitionSpec as P

AW = 1024
RANK = 128

TOKEN_PIECES = 4
PIECES = 2
EXTRA = 1
EARLY = 3
VMEM_LIMIT = 59 * 1024 * 1024


first_decay = 0.8
second_decay = 0.9
learning_rate = 0.02
norm_epsilon = 1e-06
contract_leading = (((0,), (0,)), ((), ()))


def moments(projected, first_old, second_old, clip_factor):
    scaled = clip_factor * projected
    first_new = first_decay * first_old + (1.0 - first_decay) * scaled
    second_new = second_decay * second_old + (1.0 - second_decay) * scaled * scaled
    return (first_new, second_new, first_new / jnp.sqrt(second_new))


def split_product(reduced, other):
    upper = reduced.astype(jnp.bfloat16)
    lower = (reduced - upper.astype(jnp.float32)).astype(jnp.bfloat16)
    rank_count = reduced.shape[1]
    stacked = jnp.concatenate([upper, lower], axis=1)
    both = lax.dot_general(stacked, other, contract_leading, preferred_element_type=jnp.float32)
    return both[:rank_count] + both[rank_count:]


def local(
    saved_hidden,
    grad_value,
    saved_mixed,
    grad_output,
    basis_value,
    basis_output,
    weight_value,
    weight_output,
    first_value,
    second_value,
    first_output,
    second_output,
):
    row_count = weight_value.shape[0]
    moment_count = first_value.shape[0]
    fs_index = lax.axis_index("fs")
    row_first = fs_index * row_count
    moment_first = fs_index * moment_count
    value_basis_rows = lax.dynamic_slice_in_dim(basis_value, row_first, row_count, 0).astype(
        jnp.float32
    )
    output_basis_rows = lax.dynamic_slice_in_dim(basis_output, row_first, row_count, 0).astype(
        jnp.float32
    )
    reduced_hidden = jnp.dot(saved_hidden, basis_value, preferred_element_type=jnp.float32)
    reduced_output = jnp.dot(grad_output, basis_output, preferred_element_type=jnp.float32)
    part_value = split_product(reduced_hidden, grad_value)
    part_output = split_product(reduced_output, saved_mixed)
    projected_value, projected_output = lax.psum((part_value, part_output), ("fs", "rep"))
    local_squares = jnp.sum(projected_value * projected_value) + jnp.sum(
        projected_output * projected_output
    )
    total_squares = lax.psum(local_squares, "tp")
    mean_square = total_squares / (2 * RANK * AW)
    clip_factor = jnp.minimum(1.0, 1.0 / jnp.sqrt(mean_square + norm_epsilon))
    value_slice = lax.dynamic_slice_in_dim(projected_value, moment_first, moment_count, 0)
    output_slice = lax.dynamic_slice_in_dim(projected_output, moment_first, moment_count, 0)
    new_first_value, new_second_value, value_direction_rows = moments(
        value_slice, first_value, second_value, clip_factor
    )
    new_first_output, new_second_output, output_direction_rows = moments(
        output_slice, first_output, second_output, clip_factor
    )
    direction_value, direction_output = (
        lax.all_gather(value_direction_rows, "fs", axis=0, tiled=True),
        lax.all_gather(output_direction_rows, "fs", axis=0, tiled=True),
    )
    step_value = jnp.dot(value_basis_rows, direction_value, precision=lax.Precision.HIGHEST)
    step_output = jnp.dot(output_basis_rows, direction_output, precision=lax.Precision.HIGHEST).T
    new_weight_value = weight_value - learning_rate * step_value
    new_weight_output = weight_output - learning_rate * step_output
    copy_value, copy_output = (
        lax.all_gather(new_weight_value.astype(jnp.bfloat16), "fs", axis=0, tiled=True),
        lax.all_gather(new_weight_output.astype(jnp.bfloat16), "fs", axis=1, tiled=True),
    )
    return (
        step_value,
        step_output,
        new_weight_value,
        new_weight_output,
        copy_value,
        copy_output,
        new_first_value,
        new_second_value,
        new_first_output,
        new_second_output,
    )


MESH = pl.DeviceIdType.MESH


def remote(src, dst, send, recv, **where):
    return pltpu.make_async_remote_copy(
        src_ref=src, dst_ref=dst, send_sem=send, recv_sem=recv, device_id=where, device_id_type=MESH
    )


def exchange(
    fs_count, rep_count, tp_count,
    hidden, grad_value, mixed, grad_output, basis_value, basis_output, weight_value, weight_output,
    first_value, second_value, first_output, second_output,
    step_value, step_output, new_value, new_output, copy_value, copy_output,
    new_first_value, new_second_value, new_first_output, new_second_output,
    tokens_in, thin_in, basis_in, value_in, output_in, moment_in, all_value, all_output,
    part, part_sent, landed, squares_all, owned, direction,
    load_sem, near_send, near_recv, side_send, side_recv, part_send, part_recv,
    square_send, square_recv, owned_send, owned_recv, turn_send, turn_recv, ready,
):
    group = fs_count * rep_count
    everyone = group * tp_count
    fs, rep, tp = lax.axis_index("fs"), lax.axis_index("rep"), lax.axis_index("tp")
    me = fs * rep_count + rep
    tokens = hidden.shape[0]
    count, width = value_in.shape
    rows = part.shape[2]
    piece = tokens // TOKEN_PIECES
    f32, bf16 = jnp.float32, jnp.bfloat16

    loads = []

    def load(source, target):
        copy = pltpu.make_async_copy(source, target, load_sem.at[len(loads)])
        copy.start()
        loads.append(copy)
        return copy

    weight_loads = [load(weight_value, value_in), load(weight_output, output_in)]
    stream_loads = []
    for a, (big, thin, basis) in enumerate(
        ((hidden, grad_value, basis_value), (grad_output, mixed, basis_output))
    ):
        first = [load(basis, basis_in.at[a]), load(thin, thin_in.at[a])]
        blocks = [
            load(big.at[pl.ds(c * piece, piece)], tokens_in.at[a, pl.ds(c * piece, piece)])
            for c in range(TOKEN_PIECES)
        ]
        stream_loads.append((first, blocks))
    moment_loads = [
        load(source, moment_in.at[i])
        for i, source in enumerate((first_value, first_output, second_value, second_output))
    ]

    def member(k):
        other = lax.rem(me + k, group)
        return {"fs": other // rep_count, "rep": lax.rem(other, rep_count)}

    def anyone(k):
        other = lax.rem(me * tp_count + tp + k, everyone)
        at = other // tp_count
        return {"fs": at // rep_count, "rep": lax.rem(at, rep_count), "tp": lax.rem(other, tp_count)}

    def signal(sem, **where):
        pl.semaphore_signal(sem, inc=1, device_id=where, device_id_type=MESH)

    has_next = (fs > 0, fs < fs_count - 1)

    def signal_beside(sem):
        for there, step in zip(has_next, (-1, 1)):
            @pl.when(there)
            def _():
                signal(sem, fs=fs + step)

    beside = has_next[0].astype(jnp.int32) + has_next[1].astype(jnp.int32)
    barrier = pltpu.get_barrier_semaphore()
    signal_beside(barrier)
    for j in range(1, rep_count):
        signal(barrier, rep=lax.rem(rep + j, rep_count))
    for j in range(1, tp_count):
        signal(barrier, tp=lax.rem(tp + j, tp_count))

    for copy in weight_loads:
        copy.wait()
    all_value[fs] = value_in[...].astype(bf16)
    all_output[fs] = output_in[...].astype(bf16)
    pl.semaphore_wait(barrier, beside + (rep_count - 1 + tp_count - 1))
    for j in range(1, rep_count):
        signal(ready.at[0], rep=lax.rem(rep + j, rep_count))

    def meet(k):
        if k == 0:
            pl.semaphore_wait(ready.at[0], rep_count - 1)
        else:
            pl.semaphore_wait(ready.at[k], beside)
        if k + 1 < fs_count:
            signal_beside(ready.at[k + 1])

    buffers = (all_value, all_output)
    spans = (count // (rep_count * PIECES), width // (rep_count * PIECES))

    def spot(f, s, a, q):
        owner = rep if s == 0 else lax.rem(rep + s, rep_count)
        start = pl.multiple_of((owner * PIECES + q) * spans[a], spans[a])
        return buffers[a].at[f, pl.ds(start, spans[a])]

    own_items = [(0, a, q) for a in range(2) for q in range(PIECES)]
    far_items = [(1, 1, q) for q in range(EXTRA)]
    rest_items = [(1, a, q) for a in range(2) for q in range(PIECES) if (1, a, q) not in far_items]

    def both(x, y):
        return jnp.logical_and(x, y)

    def onward(way):
        return has_next[1] if way == 0 else has_next[0]

    def reaches(way, d):
        return fs >= d if way == 0 else fs + d < fs_count

    def outer(way, d):
        return fs == d if way == 0 else fs == fs_count - 1 - d

    def comes(way, d, item):
        if item in own_items:
            return reaches(way, d)
        if item in far_items or d <= 1:
            return outer(way, d)
        return None

    def goes(way, d, item):
        if item in rest_items and d > 0:
            return None
        there = comes(way, d, item)
        return both(onward(way), there)

    def crosses(way, d, item):
        _, a, q = item
        if d == 1 or (1, a, q) in far_items:
            if d == fs_count - 1:
                return None
            return both(reaches(way, d), jnp.logical_not(outer(way, d)))
        return reaches(way, d)

    def step_of(way):
        return 1 if way == 0 else -1

    def hop(way, d, item):
        s, a, q = item
        block = spot(fs - step_of(way) * d, s, a, q)
        at = (way, d, s, a, q)
        return remote(block, block, near_send.at[at], near_recv.at[at], fs=fs + step_of(way))

    def arrival(way, d, item):
        s, a, q = item
        block = spot(fs - step_of(way) * d, s, a, q)
        at = (way, d - 1, s, a, q)
        return remote(block, block, near_send.at[at], near_recv.at[at], fs=fs - step_of(way))

    def across(way, d, item, s=0):
        _, a, q = item
        block = spot(fs - step_of(way) * d, s, a, q)
        at = (way, d - 1, a, q)
        return remote(
            block, block, side_send.at[at], side_recv.at[at], rep=lax.rem(rep + 1, rep_count)
        )

    later = []

    def send_when(there, make):
        @pl.when(there)
        def _():
            make().start()

        later.append((there, make))

    def send_own(items):
        for item in items:
            for way in range(2):
                there = goes(way, 0, item)
                send_when(there, functools.partial(hop, way, 0, item))

    def pass_on(d, items):
        for item in items:
            for way in range(2):
                there = comes(way, d, item)
                if there is None:
                    continue

                @pl.when(there)
                def _():
                    arrival(way, d, item).wait_recv()

                if d < fs_count - 1:
                    onwards = goes(way, d, item)
                    if onwards is not None:
                        send_when(onwards, functools.partial(hop, way, d, item))
                if item in own_items:
                    over = crosses(way, d, item)
                    if over is not None:
                        send_when(over, functools.partial(across, way, d, item))

    sent = []

    def send(copy):
        copy.start()
        sent.append(copy)
        return copy

    parts = []

    def send_part(a, total):
        part[a] = total.reshape(group, rows, width)
        part_sent[a] = total.astype(bf16).reshape(group, rows, width)
        for k in range(1, group):
            other = lax.rem(me + k, group)
            parts.append(send(remote(
                part_sent.at[a, other], landed.at[a, k - 1],
                part_send.at[a, k - 1], part_recv.at[a, k - 1], **member(k),
            )))

    send_own(own_items[:EARLY])
    totals = [None, None]
    pending = None

    def finish_piece(a, c, reduced):
        product = split_product(reduced, thin_in[a, pl.ds(c * piece, piece)])
        totals[a] = product if totals[a] is None else totals[a] + product

    met = 0
    for a in range(2):
        first, blocks = stream_loads[a]
        for copy in first:
            copy.wait()
        for c in range(TOKEN_PIECES):
            blocks[c].wait()
            reduced = jnp.dot(
                tokens_in[a, pl.ds(c * piece, piece)], basis_in[a], preferred_element_type=f32
            )
            if pending is not None:
                finish_piece(*pending)
                if pending[1] == TOKEN_PIECES - 1:
                    while met < fs_count:
                        meet(met)
                        met += 1
                    send_part(pending[0], totals[pending[0]])
                    send_own(own_items[EARLY:])
            pending = (a, c, reduced)
            if met < fs_count:
                meet(met)
                met += 1
    finish_piece(*pending)
    send_part(1, totals[1])
    send_own(far_items + rest_items)

    pass_on(1, own_items + far_items)
    for copy in parts:
        copy.wait_recv()
    squares = jnp.zeros((rows, width), f32)
    for a in range(2):
        summed = part[a, me]
        for k in range(group - 1):
            summed = summed + landed[a, k].astype(f32)
        owned[rep, a] = summed
        squares = squares + summed * summed
    place = me * tp_count + tp
    squares_all[place] = jnp.full(squares_all.shape[1:], jnp.sum(squares), f32)
    square_copies = [
        send(remote(
            squares_all.at[place], squares_all.at[place],
            square_send.at[k - 1], square_recv.at[k - 1], **anyone(k),
        ))
        for k in range(1, everyone)
    ]
    owned_copies = [
        send(remote(
            owned.at[rep], owned.at[rep], owned_send.at[j - 1], owned_recv.at[j - 1],
            rep=lax.rem(rep + j, rep_count),
        ))
        for j in range(1, rep_count)
    ]
    for d in range(2, fs_count - 1):
        pass_on(d, own_items)
    for copy in moment_loads:
        copy.wait()
    for copy in square_copies:
        copy.wait_recv()
    mean_square = jnp.sum(squares_all[...], axis=0) / (2 * RANK * AW)
    factor = jnp.minimum(1.0, 1.0 / jnp.sqrt(mean_square + norm_epsilon))
    scale = factor[:1, :1]
    mine_rows = pl.ds(pl.multiple_of(rep * rows, rows), rows)
    for a in range(2):
        _, _, turned = moments(
            owned[rep, a], moment_in[a, mine_rows], moment_in[2 + a, mine_rows], scale
        )
        direction[me, a] = turned.astype(bf16)
    turn_copies = [
        send(remote(
            direction.at[me], direction.at[me], turn_send.at[k - 1], turn_recv.at[k - 1], **member(k)
        ))
        for k in range(1, group)
    ]
    for d in range(2, fs_count - 1):
        pass_on(d, far_items)
    pass_on(fs_count - 1, own_items + far_items)
    for copy in owned_copies:
        copy.wait_recv()
    firsts, seconds = (new_first_value, new_first_output), (new_second_value, new_second_output)
    for a in range(2):
        projected = owned[:, a].reshape(firsts[a].shape)
        firsts[a][...], seconds[a][...], _ = moments(
            projected, moment_in[a], moment_in[2 + a], scale
        )
    for copy in turn_copies:
        copy.wait_recv()

    over = (((1,), (1,)), ((), ()))
    turn_value = direction[:, 0].reshape(RANK, width)
    turn_output = direction[:, 1].reshape(RANK, width).astype(f32).T.astype(bf16)

    def here(f):
        return pl.ds(pl.multiple_of(f * count, count), count)

    def value_step(f):
        return jnp.dot(basis_in[0, here(f)], turn_value, preferred_element_type=f32)

    def output_step(f):
        return lax.dot_general(turn_output, basis_in[1, here(f)], over, preferred_element_type=f32)

    def move(weight, step):
        return (weight.astype(f32) - learning_rate * step).astype(bf16)

    step = value_step(fs)
    step_value[...] = step
    new_value[...] = value_in[...] - learning_rate * step
    copy_value[here(fs)] = move(all_value[fs], step)
    step = output_step(fs)
    step_output[...] = step
    new_output[...] = output_in[...] - learning_rate * step
    copy_output[:, here(fs)] = move(all_output[fs], step)

    for d in range(1, fs_count):
        for a in range(2):
            for way in range(2):
                if d == 1:
                    pass_on_rest = [item for item in rest_items if item[1] == a]
                    for item in pass_on_rest:
                        @pl.when(comes(way, d, item))
                        def _():
                            arrival(way, d, item).wait_recv()
                for item in own_items:
                    if item[1] == a:
                        there = crosses(way, d, item)
                        if there is not None:
                            @pl.when(there)
                            def _():
                                across(way, d, item, 1).wait_recv()

                @pl.when(reaches(way, d))
                def _():
                    f = fs - step_of(way) * d
                    if a == 0:
                        copy_value[here(f)] = move(all_value[f], value_step(f))
                    else:
                        copy_output[:, here(f)] = move(all_output[f], output_step(f))

    for copy in sent:
        copy.wait_send()
    for there, make in later:
        @pl.when(there)
        def _():
            make().wait_send()


def finish(*refs):
    made = len(refs) // 2
    sources, targets, sem = refs[:made], refs[made : 2 * made], refs[-1]
    copies = [
        pltpu.make_async_copy(sources[i], targets[i], sem.at[i]) for i in range(made)
    ]
    for copy in copies:
        copy.start()
    for copy in copies:
        copy.wait()


def kernels(
    fs_count, rep_count, tp_count,
    saved_hidden, grad_value, saved_mixed, grad_output, basis_value, basis_output,
    weight_value, weight_output, first_value, second_value, first_output, second_output,
):
    group = fs_count * rep_count
    tokens, model = saved_hidden.shape
    count, width = weight_value.shape
    rank = basis_value.shape[1]
    rows = rank // group
    f32, bf16 = jnp.float32, jnp.bfloat16
    dma = pltpu.SemaphoreType.DMA
    anywhere = pl.BlockSpec(memory_space=pl.ANY)
    in_vmem = pl.BlockSpec(memory_space=pltpu.VMEM)
    moment = (first_value.shape, f32)
    results = (
        ((count, width), f32), ((width, count), f32), ((count, width), f32), ((width, count), f32),
        ((model, width), bf16), ((width, model), bf16), moment, moment, moment, moment,
    )
    hops = (2, fs_count - 1, rep_count, 2, PIECES)
    sides = (2, fs_count - 1, 2, PIECES)
    made = pl.pallas_call(
        functools.partial(exchange, fs_count, rep_count, tp_count),
        out_shape=tuple(pltpu.VMEM(*x) for x in results),
        in_specs=[anywhere] * 12,
        out_specs=(in_vmem,) * len(results),
        scratch_shapes=[
            pltpu.VMEM((2, tokens, model), bf16),
            pltpu.VMEM((2, tokens, width), bf16),
            pltpu.VMEM((2, model, rank), bf16),
            pltpu.VMEM((count, width), f32),
            pltpu.VMEM((width, count), f32),
            pltpu.VMEM((4,) + first_value.shape, f32),
            pltpu.VMEM((fs_count, count, width), bf16),
            pltpu.VMEM((fs_count, width, count), bf16),
            pltpu.VMEM((2, group, rows, width), f32),
            pltpu.VMEM((2, group, rows, width), bf16),
            pltpu.VMEM((2, group - 1, rows, width), bf16),
            pltpu.VMEM((group * tp_count, 1, 128), f32),
            pltpu.VMEM((rep_count, 2, rows, width), f32),
            pltpu.VMEM((group, 2, rows, width), bf16),
            dma((10 + 2 * TOKEN_PIECES,)),
            dma(hops), dma(hops), dma(sides), dma(sides),
            dma((2, group - 1)), dma((2, group - 1)),
            dma((group * tp_count - 1,)), dma((group * tp_count - 1,)),
            dma((rep_count - 1,)), dma((rep_count - 1,)),
            dma((group - 1,)), dma((group - 1,)),
            pltpu.SemaphoreType.REGULAR((fs_count,)),
        ],
        compiler_params=pltpu.CompilerParams(
            collective_id=0, has_side_effects=True, vmem_limit_bytes=VMEM_LIMIT
        ),
        name="exchange",
    )(
        saved_hidden, grad_value, saved_mixed, grad_output, basis_value, basis_output,
        weight_value, weight_output, first_value, second_value, first_output, second_output,
    )
    return pl.pallas_call(
        finish,
        out_shape=tuple(jax.ShapeDtypeStruct(*x) for x in results),
        in_specs=[anywhere] * len(results),
        out_specs=(anywhere,) * len(results),
        scratch_shapes=[dma((len(results),))],
        compiler_params=pltpu.CompilerParams(vmem_limit_bytes=1024 * 1024),
        name="finish",
    )(*made)


def solution(mesh):
    fs_count, rep_count, tp_count = mesh.shape["fs"], mesh.shape["rep"], mesh.shape["tp"]
    whole_tiles = RANK % (16 * fs_count * rep_count) == 0 and rep_count == 2 and fs_count > 2
    body = functools.partial(kernels, fs_count, rep_count, tp_count) if whole_tiles else local
    return jax.shard_map(
        body,
        mesh=mesh,
        in_specs=(
            P(("fs", "rep"), None),
            P(("fs", "rep"), "tp"),
            P(("fs", "rep"), "tp"),
            P(("fs", "rep"), None),
            P(),
            P(),
            P("fs", "tp"),
            P("tp", "fs"),
            P("fs", "tp"),
            P("fs", "tp"),
            P("fs", "tp"),
            P("fs", "tp"),
        ),
        out_specs=(
            P("fs", "tp"),
            P("tp", "fs"),
            P("fs", "tp"),
            P("tp", "fs"),
            P(None, "tp"),
            P("tp", None),
            P("fs", "tp"),
            P("fs", "tp"),
            P("fs", "tp"),
            P("fs", "tp"),
        ),
        check_vma=False,
    )
```

```python
import functools
import jax
import jax.numpy as jnp
from jax import lax
from jax.experimental import pallas as pl
from jax.experimental.pallas import tpu as pltpu
from jax.sharding import PartitionSpec as P

AW = 1024
RANK = 128

TOKEN_PIECES = 4
PIECES = 2
EXTRA = 1
EARLY = 4
AHEAD = 4
LATE = 4
VMEM_LIMIT = 59 * 1024 * 1024
MEETINGS = 3
MEET_AT = (1, 3, 5)


first_decay = 0.8
second_decay = 0.9
learning_rate = 0.02
norm_epsilon = 1e-06
contract_leading = (((0,), (0,)), ((), ()))


def moments(projected, first_old, second_old, clip_factor):
    scaled = clip_factor * projected
    first_new = first_decay * first_old + (1.0 - first_decay) * scaled
    second_new = second_decay * second_old + (1.0 - second_decay) * scaled * scaled
    return (first_new, second_new, first_new / jnp.sqrt(second_new))


def split_product(reduced, other):
    upper = reduced.astype(jnp.bfloat16)
    lower = (reduced - upper.astype(jnp.float32)).astype(jnp.bfloat16)
    rank_count = reduced.shape[1]
    stacked = jnp.concatenate([upper, lower], axis=1)
    both = lax.dot_general(stacked, other, contract_leading, preferred_element_type=jnp.float32)
    return both[:rank_count] + both[rank_count:]


def local(
    saved_hidden,
    grad_value,
    saved_mixed,
    grad_output,
    basis_value,
    basis_output,
    weight_value,
    weight_output,
    first_value,
    second_value,
    first_output,
    second_output,
):
    row_count = weight_value.shape[0]
    moment_count = first_value.shape[0]
    fs_index = lax.axis_index("fs")
    row_first = fs_index * row_count
    moment_first = fs_index * moment_count
    value_basis_rows = lax.dynamic_slice_in_dim(basis_value, row_first, row_count, 0).astype(
        jnp.float32
    )
    output_basis_rows = lax.dynamic_slice_in_dim(basis_output, row_first, row_count, 0).astype(
        jnp.float32
    )
    reduced_hidden = jnp.dot(saved_hidden, basis_value, preferred_element_type=jnp.float32)
    reduced_output = jnp.dot(grad_output, basis_output, preferred_element_type=jnp.float32)
    part_value = split_product(reduced_hidden, grad_value)
    part_output = split_product(reduced_output, saved_mixed)
    projected_value, projected_output = lax.psum((part_value, part_output), ("fs", "rep"))
    local_squares = jnp.sum(projected_value * projected_value) + jnp.sum(
        projected_output * projected_output
    )
    total_squares = lax.psum(local_squares, "tp")
    mean_square = total_squares / (2 * RANK * AW)
    clip_factor = jnp.minimum(1.0, 1.0 / jnp.sqrt(mean_square + norm_epsilon))
    value_slice = lax.dynamic_slice_in_dim(projected_value, moment_first, moment_count, 0)
    output_slice = lax.dynamic_slice_in_dim(projected_output, moment_first, moment_count, 0)
    new_first_value, new_second_value, value_direction_rows = moments(
        value_slice, first_value, second_value, clip_factor
    )
    new_first_output, new_second_output, output_direction_rows = moments(
        output_slice, first_output, second_output, clip_factor
    )
    direction_value, direction_output = (
        lax.all_gather(value_direction_rows, "fs", axis=0, tiled=True),
        lax.all_gather(output_direction_rows, "fs", axis=0, tiled=True),
    )
    step_value = jnp.dot(value_basis_rows, direction_value, precision=lax.Precision.HIGHEST)
    step_output = jnp.dot(output_basis_rows, direction_output, precision=lax.Precision.HIGHEST).T
    new_weight_value = weight_value - learning_rate * step_value
    new_weight_output = weight_output - learning_rate * step_output
    copy_value, copy_output = (
        lax.all_gather(new_weight_value.astype(jnp.bfloat16), "fs", axis=0, tiled=True),
        lax.all_gather(new_weight_output.astype(jnp.bfloat16), "fs", axis=1, tiled=True),
    )
    return (
        step_value,
        step_output,
        new_weight_value,
        new_weight_output,
        copy_value,
        copy_output,
        new_first_value,
        new_second_value,
        new_first_output,
        new_second_output,
    )


MESH = pl.DeviceIdType.MESH


def remote(src, dst, send, recv, **where):
    return pltpu.make_async_remote_copy(
        src_ref=src, dst_ref=dst, send_sem=send, recv_sem=recv, device_id=where, device_id_type=MESH
    )


def exchange(
    fs_count, rep_count, tp_count,
    hidden, grad_value, mixed, grad_output, basis_value, basis_output, weight_value, weight_output,
    first_value, second_value, first_output, second_output,
    *refs,
):
    targets, made, refs = refs[:10], refs[10:20], refs[20:]
    (
    tokens_in, thin_in, basis_in, value_in, output_in, moment_in, all_value, all_output,
    part, part_sent, landed, squares_all, owned, direction,
    load_sem, sent_sem, near_recv, side_recv, part_recv, square_recv, owned_recv, turn_recv,
    ready, store_sem,
    ) = refs
    step_value, step_output, new_value, new_output, copy_value, copy_output = made[:6]
    group = fs_count * rep_count
    everyone = group * tp_count
    fs, rep, tp = lax.axis_index("fs"), lax.axis_index("rep"), lax.axis_index("tp")
    me = fs * rep_count + rep
    at_end = jnp.logical_or(fs == 0, fs == fs_count - 1)
    tokens = hidden.shape[0]
    count, width = value_in.shape
    rows = part.shape[2]
    piece = tokens // TOKEN_PIECES
    f32, bf16 = jnp.float32, jnp.bfloat16

    stores = []

    def store(i, here=None, there=None):
        def make():
            source, target = made[i], targets[i]
            if here is not None:
                source, target = source.at[here], target.at[here]
            return pltpu.make_async_copy(source, target, store_sem)

        if there is None:
            make().start()
        else:
            @pl.when(there)
            def _():
                make().start()
        stores.append((there, make))

    loads = []

    def load(source, target):
        copy = pltpu.make_async_copy(source, target, load_sem.at[len(loads)])
        copy.start()
        loads.append(copy)
        return copy

    weight_loads = [load(weight_value, value_in), load(weight_output, output_in)]
    stream_loads = []
    for a, (big, thin, basis) in enumerate(
        ((hidden, grad_value, basis_value), (grad_output, mixed, basis_output))
    ):
        first = [load(basis, basis_in.at[a]), load(thin, thin_in.at[a])]
        blocks = [
            load(big.at[pl.ds(c * piece, piece)], tokens_in.at[a, pl.ds(c * piece, piece)])
            for c in range(TOKEN_PIECES)
        ]
        stream_loads.append((first, blocks))
    moment_loads = [
        load(source, moment_in.at[i])
        for i, source in enumerate((first_value, first_output, second_value, second_output))
    ]

    def member(k):
        other = lax.rem(me + k, group)
        return {"fs": other // rep_count, "rep": lax.rem(other, rep_count)}

    def anyone(k):
        other = lax.rem(me * tp_count + tp + k, everyone)
        at = other // tp_count
        return {"fs": at // rep_count, "rep": lax.rem(at, rep_count), "tp": lax.rem(other, tp_count)}

    def signal(sem, **where):
        pl.semaphore_signal(sem, inc=1, device_id=where, device_id_type=MESH)

    has_next = (fs > 0, fs < fs_count - 1)

    def signal_beside(sem):
        for there, step in zip(has_next, (-1, 1)):
            @pl.when(there)
            def _():
                signal(sem, fs=fs + step)

    beside = has_next[0].astype(jnp.int32) + has_next[1].astype(jnp.int32)
    barrier = pltpu.get_barrier_semaphore()
    signal_beside(barrier)
    for j in range(1, rep_count):
        signal(barrier, rep=lax.rem(rep + j, rep_count))
    for j in range(1, tp_count):
        signal(barrier, tp=lax.rem(tp + j, tp_count))

    pl.semaphore_wait(barrier, beside + (rep_count - 1 + tp_count - 1))
    signal_beside(ready.at[0])
    for j in range(1, rep_count):
        signal(ready.at[0], rep=lax.rem(rep + j, rep_count))
    inputs, buffers = (value_in, output_in), (all_value, all_output)

    def cast(owner_rep):
        for a in range(2):
            share = inputs[a].shape[0] // rep_count
            here = pl.ds(pl.multiple_of(owner_rep * share, share), share)
            buffers[a][fs, here] = inputs[a][here].astype(bf16)

    for copy in weight_loads:
        copy.wait()
    cast(rep)

    def meet(k):
        pl.semaphore_wait(ready.at[k], beside + (rep_count - 1 if k == 0 else 0))
        if k + 1 < MEETINGS:
            signal_beside(ready.at[k + 1])

    spans = (count // (rep_count * PIECES), width // (rep_count * PIECES))

    def spot(f, s, a, q):
        owner = rep if s == 0 else lax.rem(rep + s, rep_count)
        start = pl.multiple_of((owner * PIECES + q) * spans[a], spans[a])
        return buffers[a].at[f, pl.ds(start, spans[a])]

    own_items = [(0, a, q) for a in range(2) for q in range(PIECES)]
    far_items = [(1, 1, q) for q in range(EXTRA)]
    rest_items = [(1, a, q) for a in range(2) for q in range(PIECES) if (1, a, q) not in far_items]

    def both(x, y):
        return jnp.logical_and(x, y)

    def onward(way):
        return has_next[1] if way == 0 else has_next[0]

    def reaches(way, d):
        return fs >= d if way == 0 else fs + d < fs_count

    def outer(way, d):
        return fs == d if way == 0 else fs == fs_count - 1 - d

    def comes(way, d, item):
        if item in own_items:
            return reaches(way, d)
        if item in far_items or d <= 1:
            return outer(way, d)
        return None

    def goes(way, d, item):
        if item in rest_items and d > 0:
            return None
        there = comes(way, d, item)
        return both(onward(way), there)

    def crosses(way, d, item):
        _, a, q = item
        if d == 1 or (1, a, q) in far_items:
            if d == fs_count - 1:
                return None
            return both(reaches(way, d), jnp.logical_not(outer(way, d)))
        return reaches(way, d)

    def step_of(way):
        return 1 if way == 0 else -1

    def slot(block, at):
        return jnp.where(block < at, block, block - 1)

    def hop(way, d, item):
        s, a, q = item
        f, to = fs - step_of(way) * d, fs + step_of(way)
        block = spot(f, s, a, q)
        return remote(block, block, sent_sem, near_recv.at[slot(f, to), s, a, q], fs=to)

    def arrival(way, d, item):
        s, a, q = item
        f = fs - step_of(way) * d
        block = spot(f, s, a, q)
        at = near_recv.at[slot(f, fs), s, a, q]
        return remote(block, block, sent_sem, at, fs=fs - step_of(way))

    def across(way, d, item, s=0):
        _, a, q = item
        f = fs - step_of(way) * d
        block = spot(f, s, a, q)
        at = side_recv.at[slot(f, fs), a, q]
        return remote(block, block, sent_sem, at, rep=lax.rem(rep + 1, rep_count))

    later = []

    def send_when(there, make):
        @pl.when(there)
        def _():
            make().start()

        later.append((there, make))

    def send_own(items):
        for item in items:
            for way in range(2):
                there = goes(way, 0, item)
                send_when(there, functools.partial(hop, way, 0, item))

    def pass_on(d, items, only=None):
        for item in items:
            for way in range(2):
                there = comes(way, d, item)
                if there is None:
                    continue
                if only is not None:
                    there = both(there, only)

                @pl.when(there)
                def _():
                    arrival(way, d, item).wait_recv()

                if d < fs_count - 1:
                    onwards = goes(way, d, item)
                    if onwards is not None:
                        if only is not None:
                            onwards = both(onwards, only)
                        send_when(onwards, functools.partial(hop, way, d, item))
                if item in own_items:
                    over = crosses(way, d, item)
                    if over is not None:
                        if only is not None:
                            over = both(over, only)
                        send_when(over, functools.partial(across, way, d, item))

    def arrived(ref, sem):
        pltpu.make_async_copy(ref, ref, sem).wait()

    sent = []

    def send(copy):
        copy.start()
        sent.append(copy)
        return copy

    def send_part(a, total):
        part[a] = total.reshape(group, rows, width)
        part_sent[a] = total.astype(bf16).reshape(group, rows, width)
        for k in range(1, group):
            other = lax.rem(me + k, group)
            send(remote(
                part_sent.at[a, other], landed.at[a, k - 1],
                sent_sem, part_recv.at[a], **member(k),
            ))

    send_own(own_items[:EARLY])
    for j in range(1, rep_count):
        cast(lax.rem(rep + j, rep_count))
    totals = [None, None]
    pending = None

    def finish_piece(a, c, reduced):
        product = split_product(reduced, thin_in[a, pl.ds(c * piece, piece)])
        totals[a] = product if totals[a] is None else totals[a] + product

    met = 0
    for a in range(2):
        first, blocks = stream_loads[a]
        for copy in first:
            copy.wait()
        for c in range(TOKEN_PIECES):
            blocks[c].wait()
            reduced = jnp.dot(
                tokens_in[a, pl.ds(c * piece, piece)], basis_in[a], preferred_element_type=f32
            )
            if pending is not None:
                finish_piece(*pending)
            pending = (a, c, reduced)
            if a * TOKEN_PIECES + c in MEET_AT:
                meet(met)
                met += 1
                if met == MEETINGS:
                    send_part(0, totals[0])
                    send_own(own_items[EARLY:])
    finish_piece(*pending)
    send_part(1, totals[1])
    send_own(far_items + rest_items)
    pass_on(1, own_items)
    for a in range(2):
        arrived(landed.at[a], part_recv.at[a])
    squares = jnp.zeros((rows, width), f32)
    for a in range(2):
        summed = part[a, me]
        for k in range(group - 1):
            summed = summed + landed[a, k].astype(f32)
        owned[rep, a] = summed
        squares = squares + summed * summed
    place = me * tp_count + tp
    squares_all[place] = jnp.full(squares_all.shape[1:], jnp.sum(squares), f32)
    for k in range(1, everyone):
        send(remote(
            squares_all.at[place], squares_all.at[place],
            sent_sem, square_recv, **anyone(k),
        ))
    owned_copies = [
        send(remote(
            owned.at[rep], owned.at[rep], sent_sem, owned_recv.at[j - 1],
            rep=lax.rem(rep + j, rep_count),
        ))
        for j in range(1, rep_count)
    ]
    pass_on(1, far_items)
    for d in range(2, fs_count - 1):
        pass_on(d, own_items[:AHEAD])
        pass_on(d, own_items[AHEAD:], at_end)
    for copy in moment_loads:
        copy.wait()
    arrived(squares_all.at[pl.ds(0, everyone - 1)], square_recv)
    mean_square = jnp.sum(squares_all[...], axis=0) / (2 * RANK * AW)
    factor = jnp.minimum(1.0, 1.0 / jnp.sqrt(mean_square + norm_epsilon))
    scale = factor[:1, :1]
    mine_rows = pl.ds(pl.multiple_of(rep * rows, rows), rows)
    for a in range(2):
        _, _, turned = moments(
            owned[rep, a], moment_in[a, mine_rows], moment_in[2 + a, mine_rows], scale
        )
        direction[me, a] = turned.astype(bf16)
    for k in range(1, group):
        send(remote(
            direction.at[me], direction.at[me], sent_sem, turn_recv, **member(k)
        ))
    for d in range(2, fs_count - 1):
        pass_on(d, own_items[AHEAD:], jnp.logical_not(at_end))
        pass_on(d, far_items)
    pass_on(fs_count - 1, own_items[:LATE])
    arrived(direction.at[pl.ds(0, group - 1)], turn_recv)

    over = (((1,), (1,)), ((), ()))
    turn_value = direction[:, 0].reshape(RANK, width)
    turn_output = direction[:, 1].reshape(RANK, width).astype(f32).T.astype(bf16)

    def here(f):
        return pl.ds(pl.multiple_of(f * count, count), count)

    def value_step(f):
        return jnp.dot(basis_in[0, here(f)], turn_value, preferred_element_type=f32)

    def output_step(f):
        return lax.dot_general(turn_output, basis_in[1, here(f)], over, preferred_element_type=f32)

    def move(weight, step):
        return (weight.astype(f32) - learning_rate * step).astype(bf16)

    step = value_step(fs)
    step_value[...] = step
    store(0)
    new_value[...] = value_in[...] - learning_rate * step
    store(2)
    copy_value[here(fs)] = move(all_value[fs], step)
    store(4, here(fs))
    step = output_step(fs)
    step_output[...] = step
    store(1)
    new_output[...] = output_in[...] - learning_rate * step
    store(3)
    copy_output[:, here(fs)] = move(all_output[fs], step)
    store(5, (slice(None), here(fs)))

    def settle(d, a):
        for way in range(2):
            if d == 1:
                for item in rest_items:
                    if item[1] == a:
                        @pl.when(comes(way, d, item))
                        def _():
                            arrival(way, d, item).wait_recv()
            for item in own_items:
                if item[1] == a:
                    there = crosses(way, d, item)
                    if there is not None:
                        @pl.when(there)
                        def _():
                            across(way, d, item, 1).wait_recv()

            f = fs - step_of(way) * d
            at = here(f)
            held_there = reaches(way, d)

            @pl.when(held_there)
            def _():
                if a == 0:
                    copy_value[at] = move(all_value[f], value_step(f))
                else:
                    copy_output[:, at] = move(all_output[f], output_step(f))

            store(4 + a, at if a == 0 else (slice(None), at), held_there)

    for a in range(2):
        settle(1, a)
    pass_on(fs_count - 1, own_items[LATE:] + far_items)

    for copy in owned_copies:
        copy.wait_recv()
    for a in range(2):
        made[6 + 2 * a][...], made[7 + 2 * a][...], _ = moments(
            owned[:, a].reshape(moment_in.shape[1:]), moment_in[a], moment_in[2 + a], scale
        )
        store(6 + 2 * a)
        store(7 + 2 * a)
    for d in range(2, fs_count):
        for a in range(2):
            settle(d, a)

    for copy in sent:
        copy.wait_send()
    for there, make in later:
        @pl.when(there)
        def _():
            make().wait_send()

    for there, make in stores:
        if there is None:
            make().wait()
        else:
            @pl.when(there)
            def _():
                make().wait()


def finish(*refs):
    made = len(refs) // 2
    sources, targets, sem = refs[:made], refs[made : 2 * made], refs[-1]
    copies = [
        pltpu.make_async_copy(sources[i], targets[i], sem.at[i]) for i in range(made)
    ]
    for copy in copies:
        copy.start()
    for copy in copies:
        copy.wait()


def kernels(
    fs_count, rep_count, tp_count,
    saved_hidden, grad_value, saved_mixed, grad_output, basis_value, basis_output,
    weight_value, weight_output, first_value, second_value, first_output, second_output,
):
    group = fs_count * rep_count
    tokens, model = saved_hidden.shape
    count, width = weight_value.shape
    rank = basis_value.shape[1]
    rows = rank // group
    f32, bf16 = jnp.float32, jnp.bfloat16
    dma = pltpu.SemaphoreType.DMA
    anywhere = pl.BlockSpec(memory_space=pl.ANY)
    moment = (first_value.shape, f32)
    results = (
        ((count, width), f32), ((width, count), f32), ((count, width), f32), ((width, count), f32),
        ((model, width), bf16), ((width, model), bf16), moment, moment, moment, moment,
    )
    made = pl.pallas_call(
        functools.partial(exchange, fs_count, rep_count, tp_count),
        out_shape=tuple(pltpu.VMEM(*x) for x in results),
        in_specs=[anywhere] * 12,
        out_specs=(anywhere,) * len(results),
        scratch_shapes=[pltpu.VMEM(*x) for x in results]
        + [
            pltpu.VMEM((2, tokens, model), bf16),
            pltpu.VMEM((2, tokens, width), bf16),
            pltpu.VMEM((2, model, rank), bf16),
            pltpu.VMEM((count, width), f32),
            pltpu.VMEM((width, count), f32),
            pltpu.VMEM((4,) + first_value.shape, f32),
            pltpu.VMEM((fs_count, count, width), bf16),
            pltpu.VMEM((fs_count, width, count), bf16),
            pltpu.VMEM((2, group, rows, width), f32),
            pltpu.VMEM((2, group, rows, width), bf16),
            pltpu.VMEM((2, group - 1, rows, width), bf16),
            pltpu.VMEM((group * tp_count, 1, 128), f32),
            pltpu.VMEM((rep_count, 2, rows, width), f32),
            pltpu.VMEM((group, 2, rows, width), bf16),
            dma((10 + 2 * TOKEN_PIECES,)), dma,
            dma((fs_count - 1, rep_count, 2, PIECES)), dma((fs_count - 1, 2, PIECES)),
            dma((2,)), dma, dma((rep_count - 1,)), dma,
            pltpu.SemaphoreType.REGULAR((MEETINGS,)), dma,
        ],
        compiler_params=pltpu.CompilerParams(
            collective_id=0, has_side_effects=True, vmem_limit_bytes=VMEM_LIMIT
        ),
        name="exchange",
    )(
        saved_hidden, grad_value, saved_mixed, grad_output, basis_value, basis_output,
        weight_value, weight_output, first_value, second_value, first_output, second_output,
    )
    return pl.pallas_call(
        finish,
        out_shape=tuple(jax.ShapeDtypeStruct(*x) for x in results),
        in_specs=[anywhere] * len(results),
        out_specs=(anywhere,) * len(results),
        scratch_shapes=[dma((len(results),))],
        compiler_params=pltpu.CompilerParams(vmem_limit_bytes=1024 * 1024),
        name="finish",
    )(*made)


def solution(mesh):
    fs_count, rep_count, tp_count = mesh.shape["fs"], mesh.shape["rep"], mesh.shape["tp"]
    whole_tiles = rep_count == 2 and fs_count > 2 and RANK % (16 * fs_count * rep_count) == 0
    body = functools.partial(kernels, fs_count, rep_count, tp_count) if whole_tiles else local
    return jax.shard_map(
        body,
        mesh=mesh,
        in_specs=(
            P(("fs", "rep"), None),
            P(("fs", "rep"), "tp"),
            P(("fs", "rep"), "tp"),
            P(("fs", "rep"), None),
            P(),
            P(),
            P("fs", "tp"),
            P("tp", "fs"),
            P("fs", "tp"),
            P("fs", "tp"),
            P("fs", "tp"),
            P("fs", "tp"),
        ),
        out_specs=(
            P("fs", "tp"),
            P("tp", "fs"),
            P("fs", "tp"),
            P("tp", "fs"),
            P(None, "tp"),
            P("tp", None),
            P("fs", "tp"),
            P("fs", "tp"),
            P("fs", "tp"),
            P("fs", "tp"),
        ),
        check_vma=False,
    )
```

```python
import functools
import jax
import jax.numpy as jnp
from jax import lax
from jax.experimental import pallas as pl
from jax.experimental.pallas import tpu as pltpu
from jax.sharding import PartitionSpec as P

AW = 1024
RANK = 128

TOKEN_PIECES = 4
PIECES = 2
EXTRA = 1
EARLY = 4
AHEAD = 2
SOON = 1
LAST = 2
PEEK_AT = (6,)
VMEM_LIMIT = 59 * 1024 * 1024
FINISH_LIMIT = 16 * 1024 * 1024
MEETINGS = 3
MEET_AT = (1, 3, 5)


first_decay = 0.8
second_decay = 0.9
learning_rate = 0.02
norm_epsilon = 1e-06
contract_leading = (((0,), (0,)), ((), ()))


def moments(projected, first_old, second_old, clip_factor):
    scaled = clip_factor * projected
    first_new = first_decay * first_old + (1.0 - first_decay) * scaled
    second_new = second_decay * second_old + (1.0 - second_decay) * scaled * scaled
    return (first_new, second_new, first_new / jnp.sqrt(second_new))


def split_product(reduced, other):
    upper = reduced.astype(jnp.bfloat16)
    lower = (reduced - upper.astype(jnp.float32)).astype(jnp.bfloat16)
    rank_count = reduced.shape[1]
    stacked = jnp.concatenate([upper, lower], axis=1)
    both = lax.dot_general(stacked, other, contract_leading, preferred_element_type=jnp.float32)
    return both[:rank_count] + both[rank_count:]


def local(
    saved_hidden,
    grad_value,
    saved_mixed,
    grad_output,
    basis_value,
    basis_output,
    weight_value,
    weight_output,
    first_value,
    second_value,
    first_output,
    second_output,
):
    row_count = weight_value.shape[0]
    moment_count = first_value.shape[0]
    fs_index = lax.axis_index("fs")
    row_first = fs_index * row_count
    moment_first = fs_index * moment_count
    value_basis_rows = lax.dynamic_slice_in_dim(basis_value, row_first, row_count, 0).astype(
        jnp.float32
    )
    output_basis_rows = lax.dynamic_slice_in_dim(basis_output, row_first, row_count, 0).astype(
        jnp.float32
    )
    reduced_hidden = jnp.dot(saved_hidden, basis_value, preferred_element_type=jnp.float32)
    reduced_output = jnp.dot(grad_output, basis_output, preferred_element_type=jnp.float32)
    part_value = split_product(reduced_hidden, grad_value)
    part_output = split_product(reduced_output, saved_mixed)
    projected_value, projected_output = lax.psum((part_value, part_output), ("fs", "rep"))
    local_squares = jnp.sum(projected_value * projected_value) + jnp.sum(
        projected_output * projected_output
    )
    total_squares = lax.psum(local_squares, "tp")
    mean_square = total_squares / (2 * RANK * AW)
    clip_factor = jnp.minimum(1.0, 1.0 / jnp.sqrt(mean_square + norm_epsilon))
    value_slice = lax.dynamic_slice_in_dim(projected_value, moment_first, moment_count, 0)
    output_slice = lax.dynamic_slice_in_dim(projected_output, moment_first, moment_count, 0)
    new_first_value, new_second_value, value_direction_rows = moments(
        value_slice, first_value, second_value, clip_factor
    )
    new_first_output, new_second_output, output_direction_rows = moments(
        output_slice, first_output, second_output, clip_factor
    )
    direction_value, direction_output = (
        lax.all_gather(value_direction_rows, "fs", axis=0, tiled=True),
        lax.all_gather(output_direction_rows, "fs", axis=0, tiled=True),
    )
    step_value = jnp.dot(value_basis_rows, direction_value, precision=lax.Precision.HIGHEST)
    step_output = jnp.dot(output_basis_rows, direction_output, precision=lax.Precision.HIGHEST).T
    new_weight_value = weight_value - learning_rate * step_value
    new_weight_output = weight_output - learning_rate * step_output
    copy_value, copy_output = (
        lax.all_gather(new_weight_value.astype(jnp.bfloat16), "fs", axis=0, tiled=True),
        lax.all_gather(new_weight_output.astype(jnp.bfloat16), "fs", axis=1, tiled=True),
    )
    return (
        step_value,
        step_output,
        new_weight_value,
        new_weight_output,
        copy_value,
        copy_output,
        new_first_value,
        new_second_value,
        new_first_output,
        new_second_output,
    )


MESH = pl.DeviceIdType.MESH


def remote(src, dst, send, recv, **where):
    return pltpu.make_async_remote_copy(
        src_ref=src, dst_ref=dst, send_sem=send, recv_sem=recv, device_id=where, device_id_type=MESH
    )


def exchange(
    fs_count, rep_count, tp_count,
    hidden, grad_value, mixed, grad_output, basis_value, basis_output, weight_value, weight_output,
    first_value, second_value, first_output, second_output,
    direction, owned, clip, all_value, all_output, value_in, output_in, basis_in, moment_in,
    tokens_in, thin_in, part, part_sent, landed, halves, squares_all,
    load_sem, sent_sem, near_recv, side_recv, part_recv, half_recv, square_recv, turn_recv, ready,
):
    ring = fs_count * tp_count
    fs, rep, tp = lax.axis_index("fs"), lax.axis_index("rep"), lax.axis_index("tp")
    other_rep = lax.rem(rep + 1, rep_count)
    tokens = hidden.shape[0]
    count, width = value_in.shape
    rows = part.shape[2]
    piece = tokens // TOKEN_PIECES
    f32, bf16 = jnp.float32, jnp.bfloat16

    loads = []

    def load(source, target):
        copy = pltpu.make_async_copy(source, target, load_sem.at[len(loads)])
        copy.start()
        loads.append(copy)
        return copy

    weight_loads = [load(weight_value, value_in), load(weight_output, output_in)]
    stream_loads = []
    for a, (big, thin, basis) in enumerate(
        ((hidden, grad_value, basis_value), (grad_output, mixed, basis_output))
    ):
        first = [load(basis, basis_in.at[a]), load(thin, thin_in.at[a])]
        blocks = [
            load(big.at[pl.ds(c * piece, piece)], tokens_in.at[a, pl.ds(c * piece, piece)])
            for c in range(TOKEN_PIECES)
        ]
        stream_loads.append((first, blocks))
    moment_loads = [
        load(source, moment_in.at[i])
        for i, source in enumerate((first_value, first_output, second_value, second_output))
    ]

    def along(k):
        return lax.rem(fs + k, fs_count)

    def signal(sem, **where):
        pl.semaphore_signal(sem, inc=1, device_id=where, device_id_type=MESH)

    has_next = (fs > 0, fs < fs_count - 1)

    def signal_beside(sem):
        for there, step in zip(has_next, (-1, 1)):
            @pl.when(there)
            def _():
                signal(sem, fs=fs + step)

    beside = has_next[0].astype(jnp.int32) + has_next[1].astype(jnp.int32)
    barrier = pltpu.get_barrier_semaphore()
    signal_beside(barrier)
    for j in range(1, rep_count):
        signal(barrier, rep=lax.rem(rep + j, rep_count))
    for j in range(1, tp_count):
        signal(barrier, tp=lax.rem(tp + j, tp_count))

    pl.semaphore_wait(barrier, beside + (rep_count - 1 + tp_count - 1))
    signal_beside(ready.at[0])
    inputs, buffers = (value_in, output_in), (all_value, all_output)

    def cast(owner_rep):
        for a in range(2):
            share = inputs[a].shape[0] // rep_count
            here = pl.ds(pl.multiple_of(owner_rep * share, share), share)
            buffers[a][fs, here] = inputs[a][here].astype(bf16)

    for copy in weight_loads:
        copy.wait()
    cast(rep)

    def meet(k):
        pl.semaphore_wait(ready.at[k], beside)
        if k + 1 < MEETINGS:
            signal_beside(ready.at[k + 1])

    spans = (count // (rep_count * PIECES), width // (rep_count * PIECES))

    def spot(f, s, a, q):
        owner = rep if s == 0 else lax.rem(rep + s, rep_count)
        start = pl.multiple_of((owner * PIECES + q) * spans[a], spans[a])
        return buffers[a].at[f, pl.ds(start, spans[a])]

    own_items = [(0, a, q) for a in range(2) for q in range(PIECES)]
    far_items = [(1, 1, q) for q in range(EXTRA)]
    rest_items = [(1, a, q) for a in range(2) for q in range(PIECES) if (1, a, q) not in far_items]

    def both(x, y):
        return jnp.logical_and(x, y)

    def onward(way):
        return has_next[1] if way == 0 else has_next[0]

    def reaches(way, d):
        return fs >= d if way == 0 else fs + d < fs_count

    def outer(way, d):
        return fs == d if way == 0 else fs == fs_count - 1 - d

    def comes(way, d, item):
        if item in own_items:
            return reaches(way, d)
        if item in far_items or d <= 1:
            return outer(way, d)
        return None

    def goes(way, d, item):
        if item in rest_items and d > 0:
            return None
        there = comes(way, d, item)
        return both(onward(way), there)

    def crosses(way, d, item):
        _, a, q = item
        if d == 1 or (1, a, q) in far_items:
            if d == fs_count - 1:
                return None
            return both(reaches(way, d), jnp.logical_not(outer(way, d)))
        return reaches(way, d)

    def step_of(way):
        return 1 if way == 0 else -1

    def slot(block, at):
        return jnp.where(block < at, block, block - 1)

    def hop(way, d, item):
        s, a, q = item
        f, to = fs - step_of(way) * d, fs + step_of(way)
        block = spot(f, s, a, q)
        return remote(block, block, sent_sem, near_recv.at[slot(f, to), s, a, q], fs=to)

    def arrival(way, d, item):
        s, a, q = item
        f = fs - step_of(way) * d
        block = spot(f, s, a, q)
        at = near_recv.at[slot(f, fs), s, a, q]
        return remote(block, block, sent_sem, at, fs=fs - step_of(way))

    def across(way, d, item, s=0):
        _, a, q = item
        f = fs - step_of(way) * d
        block = spot(f, s, a, q)
        at = side_recv.at[slot(f, fs), a, q]
        return remote(block, block, sent_sem, at, rep=lax.rem(rep + 1, rep_count))

    later = []

    def send_when(there, make):
        @pl.when(there)
        def _():
            make().start()

        later.append((there, make))

    def send_own(items):
        for item in items:
            for way in range(2):
                there = goes(way, 0, item)
                send_when(there, functools.partial(hop, way, 0, item))

    def pass_on(d, items, only=None):
        for item in items:
            for way in range(2):
                there = comes(way, d, item)
                if there is None:
                    continue
                if only is not None:
                    there = both(there, only)

                @pl.when(there)
                def _():
                    arrival(way, d, item).wait_recv()

                if d < fs_count - 1:
                    onwards = goes(way, d, item)
                    if onwards is not None:
                        if only is not None:
                            onwards = both(onwards, only)
                        send_when(onwards, functools.partial(hop, way, d, item))
                if item in own_items:
                    over = crosses(way, d, item)
                    if over is not None:
                        if only is not None:
                            over = both(over, only)
                        send_when(over, functools.partial(across, way, d, item))

    def arrived(ref, sem):
        pltpu.make_async_copy(ref, ref, sem).wait()

    sent = []

    def send(copy):
        copy.start()
        sent.append(copy)
        return copy

    def send_part(a, total):
        part[a] = total.reshape(fs_count, rows, width)
        part_sent[a] = total.astype(bf16).reshape(fs_count, rows, width)
        for k in range(1, fs_count):
            send(remote(
                part_sent.at[a, along(k)], landed.at[a, k - 1], sent_sem, part_recv.at[a],
                fs=along(k),
            ))

    send_own(own_items[:EARLY])
    for j in range(1, rep_count):
        cast(lax.rem(rep + j, rep_count))
    totals = [None, None]
    pending = None

    def finish_piece(a, c, reduced):
        product = split_product(reduced, thin_in[a, pl.ds(c * piece, piece)])
        totals[a] = product if totals[a] is None else totals[a] + product

    met = peeked = 0
    for a in range(2):
        first, blocks = stream_loads[a]
        for copy in first:
            copy.wait()
        for c in range(TOKEN_PIECES):
            blocks[c].wait()
            reduced = jnp.dot(
                tokens_in[a, pl.ds(c * piece, piece)], basis_in[a], preferred_element_type=f32
            )
            if pending is not None:
                finish_piece(*pending)
            pending = (a, c, reduced)
            if a * TOKEN_PIECES + c in PEEK_AT:
                pass_on(1, own_items[peeked : peeked + 1])
                peeked += 1
            if a * TOKEN_PIECES + c in MEET_AT:
                meet(met)
                met += 1
                if met == MEETINGS:
                    send_part(0, totals[0])
    finish_piece(*pending)
    if met < MEETINGS:
        meet(met)
        send_part(0, totals[0])
    send_part(1, totals[1])
    send_own(own_items[EARLY:])
    send_own(far_items + rest_items)
    pass_on(1, own_items[peeked:])
    for a in range(2):
        arrived(landed.at[a], part_recv.at[a])
        summed = part[a, fs]
        for k in range(fs_count - 1):
            summed = summed + landed[a, k].astype(f32)
        halves[rep, a] = summed.astype(bf16)
        mine = halves.at[rep, a]
        send(remote(mine, mine, sent_sem, half_recv.at[a], rep=other_rep))
    pass_on(1, far_items)
    for d in range(2, fs_count - 1):
        pass_on(d, own_items[:AHEAD])
    squares = jnp.zeros((rows, width), f32)
    for a in range(2):
        arrived(halves.at[other_rep, a], half_recv.at[a])
        summed = halves[0, a].astype(f32)
        for r in range(1, rep_count):
            summed = summed + halves[r, a].astype(f32)
        owned[a] = summed
        squares = squares + summed * summed
    place = fs * tp_count + tp
    squares_all[place] = jnp.full(squares_all.shape[1:], jnp.sum(squares), f32)
    for k in range(1, ring):
        other = lax.rem(place + k, ring)
        send(remote(
            squares_all.at[place], squares_all.at[place], sent_sem, square_recv,
            fs=other // tp_count, tp=lax.rem(other, tp_count),
        ))
    for d in range(2, fs_count - 1):
        pass_on(d, own_items[AHEAD:])
        pass_on(d, far_items[:SOON])
    pass_on(fs_count - 1, own_items[:LAST])
    for copy in moment_loads:
        copy.wait()
    arrived(squares_all.at[pl.ds(0, ring - 1)], square_recv)
    mean_square = jnp.sum(squares_all[...], axis=0) / (2 * RANK * AW)
    factor = jnp.minimum(1.0, 1.0 / jnp.sqrt(mean_square + norm_epsilon))
    clip[...] = jnp.broadcast_to(factor, clip.shape)
    scale = factor[:1, :1]
    for a in range(2):
        _, _, turned = moments(owned[a], moment_in[a], moment_in[2 + a], scale)
        direction[fs, a] = turned.astype(bf16)
    for k in range(1, fs_count):
        send(remote(direction.at[fs], direction.at[fs], sent_sem, turn_recv, fs=along(k)))
    for d in range(2, fs_count - 1):
        pass_on(d, far_items[SOON:])
    pass_on(fs_count - 1, own_items[LAST:] + far_items)
    for way in range(2):
        for item in rest_items:
            @pl.when(comes(way, 1, item))
            def _():
                arrival(way, 1, item).wait_recv()
        for d in range(1, fs_count):
            for item in own_items:
                there = crosses(way, d, item)
                if there is not None:
                    @pl.when(there)
                    def _():
                        across(way, d, item, 1).wait_recv()
    arrived(direction.at[pl.ds(0, fs_count - 1)], turn_recv)

    for copy in sent:
        copy.wait_send()
    for there, make in later:
        @pl.when(there)
        def _():
            make().wait_send()


def finish(
    direction, owned, clip, all_value, all_output, value_in, output_in, basis_in, moment_in, *refs
):
    count = len(refs) // 2
    targets, made, sem = refs[:count], refs[count : 2 * count], refs[-1]
    f32, bf16 = jnp.float32, jnp.bfloat16
    fs_count, rows_each, width = all_value.shape
    fs = lax.axis_index("fs")
    over = (((1,), (1,)), ((), ()))
    stores = []

    def store(i, here=None):
        source, target = made[i], targets[i]
        if here is not None:
            source, target = source.at[here], target.at[here]
        copy = pltpu.make_async_copy(source, target, sem)
        copy.start()
        stores.append(copy)

    turn_value = direction[:, 0].reshape(RANK, width)
    turn_output = direction[:, 1].reshape(RANK, width).astype(f32).T.astype(bf16)

    def value_step(here):
        return jnp.dot(basis_in[0, here], turn_value, preferred_element_type=f32)

    def output_step(here):
        return lax.dot_general(turn_output, basis_in[1, here], over, preferred_element_type=f32)

    def move(weight, step):
        return (weight.astype(f32) - learning_rate * step).astype(bf16)

    mine = pl.ds(pl.multiple_of(fs * rows_each, rows_each), rows_each)
    step = value_step(mine)
    made[0][...] = step
    store(0)
    made[2][...] = value_in[...] - learning_rate * step
    store(2)
    step = output_step(mine)
    made[1][...] = step
    store(1)
    made[3][...] = output_in[...] - learning_rate * step
    store(3)
    for f in range(fs_count):
        here = pl.ds(f * rows_each, rows_each)
        made[4][here] = move(all_value[f], value_step(here))
        store(4, here)
    for f in range(fs_count):
        here = pl.ds(f * rows_each, rows_each)
        made[5][:, here] = move(all_output[f], output_step(here))
        store(5, (slice(None), here))
    scale = clip[:1, :1]
    for a in range(2):
        made[6 + 2 * a][...], made[7 + 2 * a][...], _ = moments(
            owned[a], moment_in[a], moment_in[2 + a], scale
        )
        store(6 + 2 * a)
        store(7 + 2 * a)
    for copy in stores:
        copy.wait()


def kernels(
    fs_count, rep_count, tp_count,
    saved_hidden, grad_value, saved_mixed, grad_output, basis_value, basis_output,
    weight_value, weight_output, first_value, second_value, first_output, second_output,
):
    tokens, model = saved_hidden.shape
    count, width = weight_value.shape
    rank = basis_value.shape[1]
    rows = rank // fs_count
    f32, bf16 = jnp.float32, jnp.bfloat16
    dma = pltpu.SemaphoreType.DMA
    anywhere = pl.BlockSpec(memory_space=pl.ANY)
    in_vmem = pl.BlockSpec(memory_space=pltpu.VMEM)
    moment = (first_value.shape, f32)
    results = (
        ((count, width), f32), ((width, count), f32), ((count, width), f32), ((width, count), f32),
        ((model, width), bf16), ((width, model), bf16), moment, moment, moment, moment,
    )
    kept = (
        ((fs_count, 2, rows, width), bf16), ((2, rows, width), f32), ((8, 128), f32),
        ((fs_count, count, width), bf16), ((fs_count, width, count), bf16),
        ((count, width), f32), ((width, count), f32),
        ((2, model, rank), bf16), ((4,) + first_value.shape, f32),
    )
    held = pl.pallas_call(
        functools.partial(exchange, fs_count, rep_count, tp_count),
        out_shape=tuple(pltpu.VMEM(*x) for x in kept),
        in_specs=[anywhere] * 12,
        out_specs=(in_vmem,) * len(kept),
        scratch_shapes=[
            pltpu.VMEM((2, tokens, model), bf16),
            pltpu.VMEM((2, tokens, width), bf16),
            pltpu.VMEM((2, fs_count, rows, width), f32),
            pltpu.VMEM((2, fs_count, rows, width), bf16),
            pltpu.VMEM((2, fs_count - 1, rows, width), bf16),
            pltpu.VMEM((rep_count, 2, rows, width), bf16),
            pltpu.VMEM((fs_count * tp_count, 1, 128), f32),
            dma((10 + 2 * TOKEN_PIECES,)), dma,
            dma((fs_count - 1, rep_count, 2, PIECES)), dma((fs_count - 1, 2, PIECES)),
            dma((2,)), dma((2,)), dma, dma,
            pltpu.SemaphoreType.REGULAR((MEETINGS,)),
        ],
        compiler_params=pltpu.CompilerParams(
            collective_id=0, has_side_effects=True, vmem_limit_bytes=VMEM_LIMIT
        ),
        name="exchange",
    )(
        saved_hidden, grad_value, saved_mixed, grad_output, basis_value, basis_output,
        weight_value, weight_output, first_value, second_value, first_output, second_output,
    )
    return pl.pallas_call(
        finish,
        out_shape=tuple(jax.ShapeDtypeStruct(*x) for x in results),
        in_specs=[in_vmem] * len(kept),
        out_specs=(anywhere,) * len(results),
        scratch_shapes=[pltpu.VMEM(*x) for x in results] + [dma],
        compiler_params=pltpu.CompilerParams(vmem_limit_bytes=FINISH_LIMIT),
        name="finish",
    )(*held)


def solution(mesh):
    fs_count, rep_count, tp_count = mesh.shape["fs"], mesh.shape["rep"], mesh.shape["tp"]
    whole_tiles = rep_count == 2 and fs_count > 2 and RANK % (16 * fs_count * rep_count) == 0
    body = functools.partial(kernels, fs_count, rep_count, tp_count) if whole_tiles else local
    return jax.shard_map(
        body,
        mesh=mesh,
        in_specs=(
            P(("fs", "rep"), None),
            P(("fs", "rep"), "tp"),
            P(("fs", "rep"), "tp"),
            P(("fs", "rep"), None),
            P(),
            P(),
            P("fs", "tp"),
            P("tp", "fs"),
            P("fs", "tp"),
            P("fs", "tp"),
            P("fs", "tp"),
            P("fs", "tp"),
        ),
        out_specs=(
            P("fs", "tp"),
            P("tp", "fs"),
            P("fs", "tp"),
            P("tp", "fs"),
            P(None, "tp"),
            P("tp", None),
            P("fs", "tp"),
            P("fs", "tp"),
            P("fs", "tp"),
            P("fs", "tp"),
        ),
        check_vma=False,
    )
```

```python
import functools
import jax
import jax.numpy as jnp
from jax import lax
from jax.experimental import pallas as pl
from jax.experimental.pallas import tpu as pltpu
from jax.sharding import PartitionSpec as P

AW = 1024
RANK = 128

TOKEN_PIECES = 4
PIECES = 2
EXTRA = 1
EARLY = 4
AHEAD = 2
SOON = 1
LAST = 2
PEEK_AT = (6,)
VMEM_LIMIT = 59 * 1024 * 1024
FINISH_LIMIT = 16 * 1024 * 1024
MEETINGS = 3
MEET_AT = (1, 3)
MIDDLE = 4


first_decay = 0.8
second_decay = 0.9
learning_rate = 0.02
norm_epsilon = 1e-06
contract_leading = (((0,), (0,)), ((), ()))


def moments(projected, first_old, second_old, clip_factor):
    scaled = clip_factor * projected
    first_new = first_decay * first_old + (1.0 - first_decay) * scaled
    second_new = second_decay * second_old + (1.0 - second_decay) * scaled * scaled
    return (first_new, second_new, first_new / jnp.sqrt(second_new))


def split_product(reduced, other):
    upper = reduced.astype(jnp.bfloat16)
    lower = (reduced - upper.astype(jnp.float32)).astype(jnp.bfloat16)
    rank_count = reduced.shape[1]
    stacked = jnp.concatenate([upper, lower], axis=1)
    both = lax.dot_general(stacked, other, contract_leading, preferred_element_type=jnp.float32)
    return both[:rank_count] + both[rank_count:]


def local(
    saved_hidden,
    grad_value,
    saved_mixed,
    grad_output,
    basis_value,
    basis_output,
    weight_value,
    weight_output,
    first_value,
    second_value,
    first_output,
    second_output,
):
    row_count = weight_value.shape[0]
    moment_count = first_value.shape[0]
    fs_index = lax.axis_index("fs")
    row_first = fs_index * row_count
    moment_first = fs_index * moment_count
    value_basis_rows = lax.dynamic_slice_in_dim(basis_value, row_first, row_count, 0).astype(
        jnp.float32
    )
    output_basis_rows = lax.dynamic_slice_in_dim(basis_output, row_first, row_count, 0).astype(
        jnp.float32
    )
    reduced_hidden = jnp.dot(saved_hidden, basis_value, preferred_element_type=jnp.float32)
    reduced_output = jnp.dot(grad_output, basis_output, preferred_element_type=jnp.float32)
    part_value = split_product(reduced_hidden, grad_value)
    part_output = split_product(reduced_output, saved_mixed)
    projected_value, projected_output = lax.psum((part_value, part_output), ("fs", "rep"))
    local_squares = jnp.sum(projected_value * projected_value) + jnp.sum(
        projected_output * projected_output
    )
    total_squares = lax.psum(local_squares, "tp")
    mean_square = total_squares / (2 * RANK * AW)
    clip_factor = jnp.minimum(1.0, 1.0 / jnp.sqrt(mean_square + norm_epsilon))
    value_slice = lax.dynamic_slice_in_dim(projected_value, moment_first, moment_count, 0)
    output_slice = lax.dynamic_slice_in_dim(projected_output, moment_first, moment_count, 0)
    new_first_value, new_second_value, value_direction_rows = moments(
        value_slice, first_value, second_value, clip_factor
    )
    new_first_output, new_second_output, output_direction_rows = moments(
        output_slice, first_output, second_output, clip_factor
    )
    direction_value, direction_output = (
        lax.all_gather(value_direction_rows, "fs", axis=0, tiled=True),
        lax.all_gather(output_direction_rows, "fs", axis=0, tiled=True),
    )
    step_value = jnp.dot(value_basis_rows, direction_value, precision=lax.Precision.HIGHEST)
    step_output = jnp.dot(output_basis_rows, direction_output, precision=lax.Precision.HIGHEST).T
    new_weight_value = weight_value - learning_rate * step_value
    new_weight_output = weight_output - learning_rate * step_output
    copy_value, copy_output = (
        lax.all_gather(new_weight_value.astype(jnp.bfloat16), "fs", axis=0, tiled=True),
        lax.all_gather(new_weight_output.astype(jnp.bfloat16), "fs", axis=1, tiled=True),
    )
    return (
        step_value,
        step_output,
        new_weight_value,
        new_weight_output,
        copy_value,
        copy_output,
        new_first_value,
        new_second_value,
        new_first_output,
        new_second_output,
    )


MESH = pl.DeviceIdType.MESH


def remote(src, dst, send, recv, **where):
    return pltpu.make_async_remote_copy(
        src_ref=src, dst_ref=dst, send_sem=send, recv_sem=recv, device_id=where, device_id_type=MESH
    )


def exchange(
    fs_count, rep_count, tp_count,
    hidden, grad_value, mixed, grad_output, basis_value, basis_output, weight_value, weight_output,
    first_value, second_value, first_output, second_output,
    direction, owned, clip, all_value, all_output, value_in, output_in, basis_in, moment_in,
    tokens_in, thin_in, part, part_sent, landed, halves, squares_all,
    load_sem, sent_sem, near_recv, side_recv, part_recv, half_recv, square_recv, turn_recv, ready,
):
    ring = fs_count * tp_count
    fs, rep, tp = lax.axis_index("fs"), lax.axis_index("rep"), lax.axis_index("tp")
    other_rep = lax.rem(rep + 1, rep_count)
    tokens = hidden.shape[0]
    count, width = value_in.shape
    rows = part.shape[2]
    piece = tokens // TOKEN_PIECES
    f32, bf16 = jnp.float32, jnp.bfloat16

    loads = []

    def load(source, target):
        copy = pltpu.make_async_copy(source, target, load_sem.at[len(loads)])
        copy.start()
        loads.append(copy)
        return copy

    weight_loads = [load(weight_value, value_in), load(weight_output, output_in)]
    stream_loads = []
    for a, (big, thin, basis) in enumerate(
        ((hidden, grad_value, basis_value), (grad_output, mixed, basis_output))
    ):
        first = [load(basis, basis_in.at[a]), load(thin, thin_in.at[a])]
        blocks = [
            load(big.at[pl.ds(c * piece, piece)], tokens_in.at[a, pl.ds(c * piece, piece)])
            for c in range(TOKEN_PIECES)
        ]
        stream_loads.append((first, blocks))
    moment_loads = [
        load(source, moment_in.at[i])
        for i, source in enumerate((first_value, first_output, second_value, second_output))
    ]

    def along(k):
        return lax.rem(fs + k, fs_count)

    def signal(sem, **where):
        pl.semaphore_signal(sem, inc=1, device_id=where, device_id_type=MESH)

    has_next = (fs > 0, fs < fs_count - 1)

    def signal_beside(sem):
        for there, step in zip(has_next, (-1, 1)):
            @pl.when(there)
            def _():
                signal(sem, fs=fs + step)

    beside = has_next[0].astype(jnp.int32) + has_next[1].astype(jnp.int32)
    barrier = pltpu.get_barrier_semaphore()
    signal_beside(barrier)
    for j in range(1, rep_count):
        signal(barrier, rep=lax.rem(rep + j, rep_count))
    for j in range(1, tp_count):
        signal(barrier, tp=lax.rem(tp + j, tp_count))

    pl.semaphore_wait(barrier, beside + (rep_count - 1 + tp_count - 1))
    signal_beside(ready.at[0])
    inputs, buffers = (value_in, output_in), (all_value, all_output)

    def cast(owner_rep):
        for a in range(2):
            share = inputs[a].shape[0] // rep_count
            here = pl.ds(pl.multiple_of(owner_rep * share, share), share)
            buffers[a][fs, here] = inputs[a][here].astype(bf16)

    for copy in weight_loads:
        copy.wait()
    cast(rep)

    def meet(k):
        pl.semaphore_wait(ready.at[k], beside)
        if k + 1 < MEETINGS:
            signal_beside(ready.at[k + 1])

    spans = (count // (rep_count * PIECES), width // (rep_count * PIECES))

    def spot(f, s, a, q):
        owner = rep if s == 0 else lax.rem(rep + s, rep_count)
        start = pl.multiple_of((owner * PIECES + q) * spans[a], spans[a])
        return buffers[a].at[f, pl.ds(start, spans[a])]

    own_items = [(0, a, q) for a in range(2) for q in range(PIECES)]
    far_items = [(1, 1, PIECES - 1 - q) for q in range(EXTRA)]
    rest_items = [(1, a, q) for a in range(2) for q in range(PIECES) if (1, a, q) not in far_items]

    def both(x, y):
        return jnp.logical_and(x, y)

    def onward(way):
        return has_next[1] if way == 0 else has_next[0]

    def reaches(way, d):
        return fs >= d if way == 0 else fs + d < fs_count

    def outer(way, d):
        return fs == d if way == 0 else fs == fs_count - 1 - d

    def comes(way, d, item):
        if item in own_items:
            return reaches(way, d)
        if item in far_items or d <= 1:
            return outer(way, d)
        return None

    def goes(way, d, item):
        if item in rest_items and d > 0:
            return None
        there = comes(way, d, item)
        return both(onward(way), there)

    def crosses(way, d, item):
        _, a, q = item
        if d == 1 or (1, a, q) in far_items:
            if d == fs_count - 1:
                return None
            return both(reaches(way, d), jnp.logical_not(outer(way, d)))
        return reaches(way, d)

    def step_of(way):
        return 1 if way == 0 else -1

    def slot(block, at):
        return jnp.where(block < at, block, block - 1)

    def hop(way, d, item):
        s, a, q = item
        f, to = fs - step_of(way) * d, fs + step_of(way)
        block = spot(f, s, a, q)
        return remote(block, block, sent_sem, near_recv.at[slot(f, to), s, a, q], fs=to)

    def arrival(way, d, item):
        s, a, q = item
        f = fs - step_of(way) * d
        block = spot(f, s, a, q)
        at = near_recv.at[slot(f, fs), s, a, q]
        return remote(block, block, sent_sem, at, fs=fs - step_of(way))

    def across(way, d, item, s=0):
        _, a, q = item
        f = fs - step_of(way) * d
        block = spot(f, s, a, q)
        at = side_recv.at[slot(f, fs), a, q]
        return remote(block, block, sent_sem, at, rep=lax.rem(rep + 1, rep_count))

    later = []

    def send_when(there, make):
        @pl.when(there)
        def _():
            make().start()

        later.append((there, make))

    def send_own(items):
        for item in items:
            for way in range(2):
                there = goes(way, 0, item)
                send_when(there, functools.partial(hop, way, 0, item))

    def pass_on(d, items, only=None):
        for item in items:
            for way in range(2):
                there = comes(way, d, item)
                if there is None:
                    continue
                if only is not None:
                    there = both(there, only)

                @pl.when(there)
                def _():
                    arrival(way, d, item).wait_recv()

                if d < fs_count - 1:
                    onwards = goes(way, d, item)
                    if onwards is not None:
                        if only is not None:
                            onwards = both(onwards, only)
                        send_when(onwards, functools.partial(hop, way, d, item))
                if item in own_items:
                    over = crosses(way, d, item)
                    if over is not None:
                        if only is not None:
                            over = both(over, only)
                        send_when(over, functools.partial(across, way, d, item))

    def arrived(ref, sem):
        pltpu.make_async_copy(ref, ref, sem).wait()

    sent = []

    def send(copy):
        copy.start()
        sent.append(copy)
        return copy

    def send_part(a, total):
        part[a] = total.reshape(fs_count, rows, width)
        part_sent[a] = total.astype(bf16).reshape(fs_count, rows, width)
        for k in range(1, fs_count):
            send(remote(
                part_sent.at[a, along(k)], landed.at[a, k - 1], sent_sem, part_recv.at[a],
                fs=along(k),
            ))

    send_own(own_items[:EARLY])
    for j in range(1, rep_count):
        cast(lax.rem(rep + j, rep_count))
    totals = [None, None]
    pending = None

    def finish_piece(a, c, reduced):
        product = split_product(reduced, thin_in[a, pl.ds(c * piece, piece)])
        totals[a] = product if totals[a] is None else totals[a] + product

    met = peeked = 0
    for a in range(2):
        first, blocks = stream_loads[a]
        for copy in first:
            copy.wait()
        for c in range(TOKEN_PIECES):
            blocks[c].wait()
            reduced = jnp.dot(
                tokens_in[a, pl.ds(c * piece, piece)], basis_in[a], preferred_element_type=f32
            )
            if pending is not None:
                finish_piece(*pending)
                if pending[1] == TOKEN_PIECES - 1:
                    send_part(0, totals[0])
                    send_own(own_items[EARLY:MIDDLE])
            pending = (a, c, reduced)
            if a * TOKEN_PIECES + c in PEEK_AT:
                pass_on(1, own_items[peeked : peeked + 1])
                peeked += 1
            if a * TOKEN_PIECES + c in MEET_AT:
                meet(met)
                met += 1
    finish_piece(*pending)
    send_part(1, totals[1])
    send_own(own_items[MIDDLE:])
    send_own(far_items + rest_items)
    pass_on(1, own_items[peeked:])
    for a in range(2):
        arrived(landed.at[a], part_recv.at[a])
        summed = part[a, fs]
        for k in range(fs_count - 1):
            summed = summed + landed[a, k].astype(f32)
        halves[rep, a] = summed.astype(bf16)
        mine = halves.at[rep, a]
        send(remote(mine, mine, sent_sem, half_recv.at[a], rep=other_rep))
    pass_on(1, far_items)
    for d in range(2, fs_count - 1):
        pass_on(d, own_items[:AHEAD])
    meet(met)
    squares = jnp.zeros((rows, width), f32)
    for a in range(2):
        arrived(halves.at[other_rep, a], half_recv.at[a])
        summed = halves[0, a].astype(f32)
        for r in range(1, rep_count):
            summed = summed + halves[r, a].astype(f32)
        owned[a] = summed
        squares = squares + summed * summed
    place = fs * tp_count + tp
    squares_all[place] = jnp.full(squares_all.shape[1:], jnp.sum(squares), f32)
    for k in range(1, ring):
        other = lax.rem(place + k, ring)
        send(remote(
            squares_all.at[place], squares_all.at[place], sent_sem, square_recv,
            fs=other // tp_count, tp=lax.rem(other, tp_count),
        ))
    for d in range(2, fs_count - 1):
        pass_on(d, own_items[AHEAD:])
        pass_on(d, far_items[:SOON])
    pass_on(fs_count - 1, own_items[:LAST])
    for copy in moment_loads:
        copy.wait()
    arrived(squares_all.at[pl.ds(0, ring - 1)], square_recv)
    mean_square = jnp.sum(squares_all[...], axis=0) / (2 * RANK * AW)
    factor = jnp.minimum(1.0, 1.0 / jnp.sqrt(mean_square + norm_epsilon))
    clip[...] = jnp.broadcast_to(factor, clip.shape)
    scale = factor[:1, :1]
    for a in range(2):
        _, _, turned = moments(owned[a], moment_in[a], moment_in[2 + a], scale)
        direction[fs, a] = turned.astype(bf16)
    for k in range(1, fs_count):
        send(remote(direction.at[fs], direction.at[fs], sent_sem, turn_recv, fs=along(k)))
    for d in range(2, fs_count - 1):
        pass_on(d, far_items[SOON:])
    pass_on(fs_count - 1, own_items[LAST:] + far_items)
    for way in range(2):
        for item in rest_items:
            @pl.when(comes(way, 1, item))
            def _():
                arrival(way, 1, item).wait_recv()
        for d in range(1, fs_count):
            for item in own_items:
                there = crosses(way, d, item)
                if there is not None:
                    @pl.when(there)
                    def _():
                        across(way, d, item, 1).wait_recv()
    arrived(direction.at[pl.ds(0, fs_count - 1)], turn_recv)

    for copy in sent:
        copy.wait_send()
    for there, make in later:
        @pl.when(there)
        def _():
            make().wait_send()


def finish(
    direction, owned, clip, all_value, all_output, value_in, output_in, basis_in, moment_in, *refs
):
    count = len(refs) // 2
    targets, made, sem = refs[:count], refs[count : 2 * count], refs[-1]
    f32, bf16 = jnp.float32, jnp.bfloat16
    fs_count, rows_each, width = all_value.shape
    fs = lax.axis_index("fs")
    over = (((1,), (1,)), ((), ()))
    stores = []

    def store(i, here=None):
        source, target = made[i], targets[i]
        if here is not None:
            source, target = source.at[here], target.at[here]
        copy = pltpu.make_async_copy(source, target, sem)
        copy.start()
        stores.append(copy)

    turn_value = direction[:, 0].reshape(RANK, width)
    turn_output = direction[:, 1].reshape(RANK, width).astype(f32).T.astype(bf16)

    def value_step(here):
        return jnp.dot(basis_in[0, here], turn_value, preferred_element_type=f32)

    def output_step(here):
        return lax.dot_general(turn_output, basis_in[1, here], over, preferred_element_type=f32)

    def move(weight, step):
        return (weight.astype(f32) - learning_rate * step).astype(bf16)

    mine = pl.ds(pl.multiple_of(fs * rows_each, rows_each), rows_each)
    step = value_step(mine)
    made[0][...] = step
    store(0)
    made[2][...] = value_in[...] - learning_rate * step
    store(2)
    step = output_step(mine)
    made[1][...] = step
    store(1)
    made[3][...] = output_in[...] - learning_rate * step
    store(3)
    for f in range(fs_count):
        here = pl.ds(f * rows_each, rows_each)
        made[4][here] = move(all_value[f], value_step(here))
        store(4, here)
    for f in range(fs_count):
        here = pl.ds(f * rows_each, rows_each)
        made[5][:, here] = move(all_output[f], output_step(here))
        store(5, (slice(None), here))
    scale = clip[:1, :1]
    for a in range(2):
        made[6 + 2 * a][...], made[7 + 2 * a][...], _ = moments(
            owned[a], moment_in[a], moment_in[2 + a], scale
        )
        store(6 + 2 * a)
        store(7 + 2 * a)
    for copy in stores:
        copy.wait()


def kernels(
    fs_count, rep_count, tp_count,
    saved_hidden, grad_value, saved_mixed, grad_output, basis_value, basis_output,
    weight_value, weight_output, first_value, second_value, first_output, second_output,
):
    tokens, model = saved_hidden.shape
    count, width = weight_value.shape
    rank = basis_value.shape[1]
    rows = rank // fs_count
    f32, bf16 = jnp.float32, jnp.bfloat16
    dma = pltpu.SemaphoreType.DMA
    anywhere = pl.BlockSpec(memory_space=pl.ANY)
    in_vmem = pl.BlockSpec(memory_space=pltpu.VMEM)
    moment = (first_value.shape, f32)
    results = (
        ((count, width), f32), ((width, count), f32), ((count, width), f32), ((width, count), f32),
        ((model, width), bf16), ((width, model), bf16), moment, moment, moment, moment,
    )
    kept = (
        ((fs_count, 2, rows, width), bf16), ((2, rows, width), f32), ((8, 128), f32),
        ((fs_count, count, width), bf16), ((fs_count, width, count), bf16),
        ((count, width), f32), ((width, count), f32),
        ((2, model, rank), bf16), ((4,) + first_value.shape, f32),
    )
    held = pl.pallas_call(
        functools.partial(exchange, fs_count, rep_count, tp_count),
        out_shape=tuple(pltpu.VMEM(*x) for x in kept),
        in_specs=[anywhere] * 12,
        out_specs=(in_vmem,) * len(kept),
        scratch_shapes=[
            pltpu.VMEM((2, tokens, model), bf16),
            pltpu.VMEM((2, tokens, width), bf16),
            pltpu.VMEM((2, fs_count, rows, width), f32),
            pltpu.VMEM((2, fs_count, rows, width), bf16),
            pltpu.VMEM((2, fs_count - 1, rows, width), bf16),
            pltpu.VMEM((rep_count, 2, rows, width), bf16),
            pltpu.VMEM((fs_count * tp_count, 1, 128), f32),
            dma((10 + 2 * TOKEN_PIECES,)), dma,
            dma((fs_count - 1, rep_count, 2, PIECES)), dma((fs_count - 1, 2, PIECES)),
            dma((2,)), dma((2,)), dma, dma,
            pltpu.SemaphoreType.REGULAR((MEETINGS,)),
        ],
        compiler_params=pltpu.CompilerParams(
            collective_id=0, has_side_effects=True, vmem_limit_bytes=VMEM_LIMIT
        ),
        name="exchange",
    )(
        saved_hidden, grad_value, saved_mixed, grad_output, basis_value, basis_output,
        weight_value, weight_output, first_value, second_value, first_output, second_output,
    )
    return pl.pallas_call(
        finish,
        out_shape=tuple(jax.ShapeDtypeStruct(*x) for x in results),
        in_specs=[in_vmem] * len(kept),
        out_specs=(anywhere,) * len(results),
        scratch_shapes=[pltpu.VMEM(*x) for x in results] + [dma],
        compiler_params=pltpu.CompilerParams(vmem_limit_bytes=FINISH_LIMIT),
        name="finish",
    )(*held)


def solution(mesh):
    fs_count, rep_count, tp_count = mesh.shape["fs"], mesh.shape["rep"], mesh.shape["tp"]
    whole_tiles = rep_count == 2 and fs_count > 2 and RANK % (16 * fs_count * rep_count) == 0
    body = functools.partial(kernels, fs_count, rep_count, tp_count) if whole_tiles else local
    return jax.shard_map(
        body,
        mesh=mesh,
        in_specs=(
            P(("fs", "rep"), None),
            P(("fs", "rep"), "tp"),
            P(("fs", "rep"), "tp"),
            P(("fs", "rep"), None),
            P(),
            P(),
            P("fs", "tp"),
            P("tp", "fs"),
            P("fs", "tp"),
            P("fs", "tp"),
            P("fs", "tp"),
            P("fs", "tp"),
        ),
        out_specs=(
            P("fs", "tp"),
            P("tp", "fs"),
            P("fs", "tp"),
            P("tp", "fs"),
            P(None, "tp"),
            P("tp", None),
            P("fs", "tp"),
            P("fs", "tp"),
            P("fs", "tp"),
            P("fs", "tp"),
        ),
        check_vma=False,
    )
```
